512 devices in a mesh: sp: 64 (over z, y), tp: 8 (over x, core).
Axes of the slice: x: 4, y: 8, z: 8, core: 2. Of those that a mesh axis runs over, the one named last changes fastest.
Arguments:
- tokens: bfloat16 [65536, 2048], P(('sp', 'tp')), may hold values from -6 to 6
- norm_gain: float32 [2048], replicated, may hold values from 0.1 to 1.9
- w_query: bfloat16 [2048, 1024], P('sp', 'tp'), may hold values from -0.125 to 0.125
- w_key: bfloat16 [2048, 1024], P('sp', 'tp'), may hold values from -0.125 to 0.125
- w_value: bfloat16 [2048, 1024], P('sp', 'tp'), may hold values from -0.125 to 0.125
- decay_rate: float32 [512, 8], P('sp', 'tp'), may hold values from 7.6293945e-07 to 0.1, as said below
- state_init: float32 [8, 128, 128], P('tp'), may hold values from -48 to 48
- out_gain: float32 [1024], P('tp'), may hold values from 0.1 to 1.9
- w_out: bfloat16 [1024, 2048], P('tp', 'sp'), may hold values from -0.1875 to 0.1875
Outputs:
- mixed: bfloat16 [65536, 2048], P(('sp', 'tp'))
The draws below stay inside these ranges and needn't reach their ends.
Inputs may be any that keep to these rules, and one draw needn't show every extreme that they name: `decay_rate`: constant over each block of 128 positions.
All inputs are finite; a program needn't handle non-finite values.
Results may differ from the reference program's by a relative error of at most 0.025.
Values may be sent and summed in bfloat16 or wider, within the bound.
No kernel may reach another device: no remote copies, remote signals or barrier semaphores. Data moves between devices by JAX's collectives and lax.ppermute only.
A program may use at most 64 MiB of HBM per device.

```python
import math
import jax
import jax.numpy as jnp
from jax import lax

D = 2048
HEADS = 8
HEAD_DIM = 128
BLOCK = 128
SEQ = 65536
RET_WIDTH = 1024
N_TP = 8


def draw_decay_rate(key, part):
    keys = jax.random.split(key, 4)
    count_blocks = SEQ // BLOCK
    fast_share = 0.5
    fast_heads = jax.random.uniform(keys[0], (HEADS,), jnp.float32) < fast_share
    slow_base = math.log(10.0) / SEQ * jnp.exp(jax.random.uniform(keys[1], (HEADS,), jnp.float32, math.log(0.15), math.log(0.5)))
    fast_base = jnp.exp(jax.random.uniform(keys[2], (HEADS,), jnp.float32, math.log(1.0 / 50.0), math.log(1.0 / 25.0)))
    factor = jnp.exp(jax.random.uniform(keys[3], (count_blocks, HEADS), jnp.float32, math.log(0.5), math.log(2.0)))
    return (jnp.where(fast_heads, fast_base, slow_base)[None, :] * factor).astype(jnp.float32)


def level_of(key, extent, pieces, smallest, high):
    def one(position, parts):
        draws = jax.random.uniform(jax.random.fold_in(jax.random.fold_in(key, 6), position), (parts,), jnp.float32, smallest / len(pieces), high / len(pieces))
        return jnp.repeat(jnp.exp(draws), extent[position] // parts).reshape((-1,) + (1,) * (len(extent) - position - 1))

    gain = one(*pieces[0])
    for cut in pieces[1:]:
        gain = gain * one(*cut)
    return gain


def scatter_about(key, shape, deviation, bound, cuts=(), kind=jnp.bfloat16):
    entries = jax.random.normal(key, shape, jnp.float32) * deviation
    if len(cuts) > 0:
        entries = level_of(key, shape, cuts, -0.22, 0.18) * entries
    return jnp.clip(entries, min=-bound, max=bound).astype(kind)


def setup_inputs(seed: int = 0) -> dict:
    seeds = jax.random.split(jax.random.key(seed), 10)
    tokens = scatter_about(seeds[0], (SEQ, D), 1.0, 6.0, ((0, 512),))
    norm_gain = jnp.clip(1.0 + 0.18 * jax.random.normal(seeds[1], (D,), jnp.float32), 0.1, 1.9)
    w_query = scatter_about(seeds[2], (D, RET_WIDTH), D ** -0.5, 0.125, ((0, 64), (1, 8)))
    w_key = scatter_about(seeds[3], (D, RET_WIDTH), D ** -0.5, 0.125, ((0, 64), (1, 8)))
    w_value = scatter_about(seeds[4], (D, RET_WIDTH), D ** -0.5, 0.125, ((0, 64), (1, 8)))
    decay_rate = draw_decay_rate(jax.random.fold_in(seeds[9], 71), 0)
    state_init = scatter_about(seeds[6], (HEADS, HEAD_DIM, HEAD_DIM), 8.0, 48.0, ((0, 8),), jnp.float32)
    out_gain = jnp.clip(1.0 + 0.18 * jax.random.normal(seeds[7], (RET_WIDTH,), jnp.float32), 0.1, 1.9)
    w_out = scatter_about(seeds[8], (RET_WIDTH, D), RET_WIDTH ** -0.5, 0.1875, ((0, 8), (1, 64)))
    return {"tokens": tokens, "norm_gain": norm_gain, "w_query": w_query, "w_key": w_key, "w_value": w_value, "decay_rate": decay_rate, "state_init": state_init, "out_gain": out_gain, "w_out": w_out}


EPS = 0.1
ROPE_BASE = 10000.0

def rotate(values_in, positions):
    half_dim = values_in.shape[-1] // 2
    inv_freq = ROPE_BASE ** (-jnp.arange(half_dim, dtype=jnp.float32) / half_dim)
    angles = positions[:, None] * inv_freq[None, :]
    cosine = jnp.cos(angles)[:, None, :]
    sine_part = jnp.sin(angles)[:, None, :]
    first_half = values_in[..., :half_dim]
    second_half = values_in[..., half_dim:]
    return jnp.concatenate([first_half * cosine - second_half * sine_part, second_half * cosine + first_half * sine_part], axis=-1)

def reference(tokens, norm_gain, w_query, w_key, w_value, decay_rate, state_init, out_gain, w_out):
    high = lax.Precision.HIGHEST
    values_in = tokens.astype(jnp.float32)
    normed = (values_in * lax.rsqrt(lax.optimization_barrier(jnp.mean(values_in * values_in, axis=-1, keepdims=True)) + EPS) * norm_gain).astype(jnp.bfloat16)
    positions = jnp.arange(SEQ, dtype=jnp.float32)
    query_rot = rotate(jnp.dot(normed, w_query, preferred_element_type=jnp.float32).reshape(SEQ, HEADS, HEAD_DIM), positions).astype(jnp.bfloat16)
    key_rot = rotate(jnp.dot(normed, w_key, preferred_element_type=jnp.float32).reshape(SEQ, HEADS, HEAD_DIM), positions).astype(jnp.bfloat16)
    value_rows = jnp.dot(normed, w_value, preferred_element_type=jnp.float32).astype(jnp.bfloat16)
    value_rows = value_rows.reshape(SEQ, HEADS, HEAD_DIM)
    count_blocks = SEQ // BLOCK
    q_blocks = query_rot.astype(jnp.float32).reshape(count_blocks, BLOCK, HEADS, HEAD_DIM)
    k_blocks = key_rot.astype(jnp.float32).reshape(count_blocks, BLOCK, HEADS, HEAD_DIM) * HEAD_DIM ** (-0.5)
    v_blocks = value_rows.astype(jnp.float32).reshape(count_blocks, BLOCK, HEADS, HEAD_DIM)
    offsets = jnp.arange(BLOCK, dtype=jnp.float32)
    step_gap = offsets[:, None] - offsets[None, :]

    def advance(state_now, block_item):
        q_one, k_one, v_one, rate_one = block_item
        inside = jnp.where(step_gap[None] >= 0.0, jnp.exp(-jnp.maximum(step_gap, 0.0)[None] * rate_one[:, None, None]), 0.0)
        scores = jnp.einsum('ihd,jhd->hij', q_one, k_one, precision=high) * inside
        inner_part = jnp.einsum('hij,jhe->ihe', scores, v_one, precision=high)
        read_decay = jnp.exp(-(offsets + 1.0)[:, None] * rate_one[None, :])
        cross_part = jnp.einsum('ihd,hde->ihe', q_one, state_now, precision=high) * read_decay[:, :, None]
        tail_decay = jnp.exp(-(BLOCK - 1.0 - offsets)[:, None] * rate_one[None, :])
        block_kv = jnp.einsum('jhd,jhe->hde', k_one * tail_decay[:, :, None], v_one, precision=high)
        state_next = jnp.exp(-BLOCK * rate_one)[:, None, None] * state_now + block_kv
        return (state_next, inner_part + cross_part)
    final_state, retained = lax.scan(advance, state_init.astype(jnp.float32), (q_blocks, k_blocks, v_blocks, decay_rate))
    out_heads = retained.reshape(SEQ, HEADS, HEAD_DIM)
    out_heads = out_heads * lax.rsqrt(lax.optimization_barrier(jnp.mean(out_heads * out_heads, axis=-1, keepdims=True)) + EPS)
    out_heads = out_heads * out_gain.reshape(HEADS, HEAD_DIM)
    hidden = out_heads.reshape(SEQ, RET_WIDTH).astype(jnp.bfloat16)
    group_cols = RET_WIDTH // N_TP
    total_sum = jnp.zeros((SEQ, D), jnp.float32)
    for group in range(N_TP):
        partial_value = jnp.dot(hidden[:, group * group_cols:(group + 1) * group_cols], w_out[group * group_cols:(group + 1) * group_cols], preferred_element_type=jnp.float32).astype(jnp.bfloat16)
        partial_value = lax.optimization_barrier(partial_value)
        total_sum = total_sum + partial_value.astype(jnp.float32)
    return total_sum.astype(jnp.bfloat16)
```

```python
import jax
import jax.numpy as jnp
from jax import lax
from jax.experimental import pallas as pl
from jax.experimental.pallas import tpu as pltpu
from jax.sharding import Mesh
from jax.sharding import PartitionSpec as P

HEAD_DIM = 128
BLOCK = 128
SP = ("sp_0", "sp_1")
TP = ("tp_0", "tp_1")
EPS = 0.1
ROPE_BASE = 10000.0

VMEM = pl.BlockSpec(memory_space=pltpu.VMEM)
SMEM = pl.BlockSpec(memory_space=pltpu.SMEM)
ANY = pl.BlockSpec(memory_space=pl.ANY)


def sent_to_all(shard, axis):
    count = lax.axis_size(axis)
    return lax.all_to_all(
        jnp.broadcast_to(shard[None], (count, *shard.shape)), axis, 0, 0, tiled=True
    )


def from_others(own):
    n = lax.axis_size("tp_0")
    same = [own]
    for d in range(1, n):
        same.append(lax.ppermute(own, "tp_0", [(i, (i + d) % n) for i in range(n)]))
    other = [lax.ppermute(v, "tp_1", [(0, 1), (1, 0)]) for v in same]
    return same + other


def norm_kernel(x_ref, gain_ref, out_ref):
    x = x_ref[...].astype(jnp.float32)
    scale = lax.rsqrt(jnp.mean(x * x, axis=-1, keepdims=True) + EPS)
    out_ref[...] = (x * scale * gain_ref[...]).astype(jnp.bfloat16)


def normalized(tokens, gain):
    return pl.pallas_call(
        norm_kernel,
        out_shape=jax.ShapeDtypeStruct(tokens.shape, jnp.bfloat16),
        in_specs=[VMEM, VMEM],
        out_specs=VMEM,
        cost_estimate=pl.CostEstimate(flops=2000000, bytes_accessed=1 << 20, transcendentals=0),
    )(tokens, gain[None])


def local_kernel(place, rates, *refs):
    count = place[2]
    xs = refs[:8]
    w_hbm, cos_ref, sin_ref, q_out, l_out, s_out = refs[8:14]
    x_buf, w_buf, k_buf, v_buf, s_buf, sems = refs[14:]
    copies = []
    w_copy = pltpu.make_async_copy(w_hbm, w_buf, sems.at[8])
    w_copy.start()
    for j in range(8):
        copies.append(pltpu.make_async_copy(xs[j], x_buf.at[pl.ds(j * BLOCK, BLOCK)], sems.at[j]))
        copies[-1].start()
    w_copy.wait()

    def start_row(j):
        here = lax.rem(place[0] - j % 4 + 4, 4)
        core = place[1] if j < 4 else 1 - place[1]
        return pl.multiple_of((here * 2 + core) * BLOCK, BLOCK)

    half = 2
    for g in range(8 // half):
        for j in range(half):
            copies[g * half + j].wait()
        raw = jnp.dot(
            x_buf[pl.ds(g * half * BLOCK, half * BLOCK), :],
            w_buf[:, : 3 * HEAD_DIM],
            preferred_element_type=jnp.float32,
        )
        for j in range(half):
            at = start_row(g * half + j)
            rows = pl.ds(at, BLOCK)
            cosine = cos_ref[rows, :]
            sine = sin_ref[rows, :]
            part = raw[j * BLOCK : (j + 1) * BLOCK, :]
            q = part[:, :HEAD_DIM]
            k = part[:, HEAD_DIM : 2 * HEAD_DIM]
            v = part[:, 2 * HEAD_DIM :]
            q = q * cosine + pltpu.roll(q, HEAD_DIM // 2, 1) * sine
            k = k * cosine + pltpu.roll(k, HEAD_DIM // 2, 1) * sine
            q_out[rows, :] = q.astype(jnp.bfloat16)
            k_buf[rows, :] = k.astype(jnp.bfloat16)
            v_buf[rows, :] = v.astype(jnp.bfloat16)

    row = lax.broadcasted_iota(jnp.int32, (BLOCK, BLOCK), 0).astype(jnp.float32)
    col = lax.broadcasted_iota(jnp.int32, (BLOCK, BLOCK), 1).astype(jnp.float32)
    gap = row - col
    scale = HEAD_DIM**-0.5
    state = jnp.zeros((HEAD_DIM, HEAD_DIM), jnp.float32)
    total = jnp.float32(0.0)
    for b in range(8):
        rate = rates[b, 0]
        total = total + rate
        rows = pl.ds(b * BLOCK, BLOCK)
        q, k, v = q_out[rows, :], k_buf[rows, :], v_buf[rows, :]
        inside = jnp.where(gap >= 0.0, jnp.exp(-jnp.maximum(gap, 0.0) * rate) * scale, 0.0)
        scores = lax.dot_general(q, k, (((1,), (1,)), ((), ())), preferred_element_type=jnp.float32)
        out = jnp.dot(
            (scores * inside).astype(jnp.bfloat16), v, preferred_element_type=jnp.float32
        )
        if b > 0:
            cross = jnp.dot(q, state.astype(jnp.bfloat16), preferred_element_type=jnp.float32)
            out = out + cross * jnp.exp(-(row + 1.0) * rate)
        l_out[rows, :] = out
        tail = jnp.exp(-(BLOCK - 1.0 - row) * rate) * scale
        fed = (k.astype(jnp.float32) * tail).astype(jnp.bfloat16)
        kv = lax.dot_general(fed, v, (((0,), (0,)), ((), ())), preferred_element_type=jnp.float32)
        state = jnp.exp(jnp.full((HEAD_DIM, HEAD_DIM), -float(BLOCK), jnp.float32) * rate) * state + kv
    s_buf[...] = state
    decay = jnp.exp(jnp.full((2, HEAD_DIM), -float(BLOCK), jnp.float32) * total)
    for i in range(64):
        s_out[i, 0:2, :] = s_buf[2 * i : 2 * i + 2, :]
        s_out[i, 2:4, :] = decay


def local_part(place, rates, chunks, weights, cosine, sine):
    span = 8 * BLOCK
    return pl.pallas_call(
        local_kernel,
        out_shape=(
            jax.ShapeDtypeStruct((span, HEAD_DIM), jnp.bfloat16),
            jax.ShapeDtypeStruct((span, HEAD_DIM), jnp.float32),
            jax.ShapeDtypeStruct((64, 4, HEAD_DIM), jnp.float32),
        ),
        in_specs=[SMEM, SMEM] + [ANY] * 9 + [VMEM, VMEM],
        out_specs=(VMEM, VMEM, VMEM),
        scratch_shapes=[
            pltpu.VMEM((span, 2048), jnp.bfloat16),
            pltpu.VMEM((2048, 512), jnp.bfloat16),
            pltpu.VMEM((span, HEAD_DIM), jnp.bfloat16),
            pltpu.VMEM((span, HEAD_DIM), jnp.bfloat16),
            pltpu.VMEM((HEAD_DIM, HEAD_DIM), jnp.float32),
            pltpu.SemaphoreType.DMA((9,)),
        ],
        compiler_params=pltpu.CompilerParams(vmem_limit_bytes=24 << 20),
        cost_estimate=pl.CostEstimate(
            flops=1700000000, bytes_accessed=7 << 20, transcendentals=1 << 18
        ),
    )(place, rates, *chunks, weights, cosine, sine)


def scan_kernel(place, got_ref, init_ref, out_ref):
    state = init_ref[place[2]]
    for s in range(64):
        out_ref[s] = state
        state = got_ref[s, 2:4, :] * state + got_ref[s, 0:2, :]


def scanned(place, got, init):
    return pl.pallas_call(
        scan_kernel,
        out_shape=jax.ShapeDtypeStruct((64, 2, HEAD_DIM), jnp.float32),
        in_specs=[SMEM, VMEM, VMEM],
        out_specs=VMEM,
        cost_estimate=pl.CostEstimate(flops=1000000, bytes_accessed=1 << 18, transcendentals=0),
    )(place, got, init)


def hidden_kernel(rates, state_ref, q_ref, l_ref, gain_ref, out_ref):
    row = lax.broadcasted_iota(jnp.int32, (BLOCK, HEAD_DIM), 0).astype(jnp.float32)
    state = state_ref[...].astype(jnp.bfloat16)
    gain = gain_ref[...]
    before = jnp.float32(0.0)
    for b in range(8):
        rate = rates[b, 0]
        rows = pl.ds(b * BLOCK, BLOCK)
        carried = jnp.dot(q_ref[rows, :], state, preferred_element_type=jnp.float32)
        mixed = l_ref[rows, :] + carried * jnp.exp(-(row + 1.0) * rate - BLOCK * before)
        norm = lax.rsqrt(jnp.mean(mixed * mixed, axis=-1, keepdims=True) + EPS)
        out_ref[b] = (mixed * norm * gain).astype(jnp.bfloat16)
        before = before + rate


def hidden_part(rates, state, q, local_out, gain):
    return pl.pallas_call(
        hidden_kernel,
        out_shape=jax.ShapeDtypeStruct((8, BLOCK, HEAD_DIM), jnp.bfloat16),
        in_specs=[SMEM] + [VMEM] * 4,
        out_specs=VMEM,
        cost_estimate=pl.CostEstimate(
            flops=40000000, bytes_accessed=1 << 20, transcendentals=1 << 17
        ),
    )(rates, state, q, local_out, gain)


def out_kernel(place, h_ref, *refs):
    ws = refs[:8]
    out_ref, w_buf, sems = refs[8:]
    copies = []
    for j in range(8):
        copies.append(pltpu.make_async_copy(ws[j], w_buf.at[j], sems.at[j]))
        copies[-1].start()
    total = None
    for j in range(8):
        here = lax.rem(place[0] - j % 4 + 4, 4)
        core = place[1] if j < 4 else 1 - place[1]
        copies[j].wait()
        part = lax.dot_general(
            h_ref[here * 2 + core],
            w_buf[j],
            (((1,), (1,)), ((), ())),
            preferred_element_type=jnp.float32,
        )
        total = part if total is None else total + part
    out_ref[...] = total.astype(jnp.bfloat16)


def out_part(place, hidden, weights):
    return pl.pallas_call(
        out_kernel,
        out_shape=jax.ShapeDtypeStruct((BLOCK, 2048), jnp.bfloat16),
        in_specs=[SMEM, VMEM] + [ANY] * 8,
        out_specs=VMEM,
        scratch_shapes=[
            pltpu.VMEM((8, 2048, HEAD_DIM), jnp.bfloat16),
            pltpu.SemaphoreType.DMA((8,)),
        ],
        compiler_params=pltpu.CompilerParams(vmem_limit_bytes=24 << 20),
        cost_estimate=pl.CostEstimate(
            flops=540000000, bytes_accessed=5 << 20, transcendentals=0
        ),
    )(place, hidden, *weights)


def rotation_tables(first, rows):
    half = HEAD_DIM // 2
    inv_freq = ROPE_BASE ** (-jnp.arange(half, dtype=jnp.float32) / half)
    positions = (first + jnp.arange(rows, dtype=jnp.int32)).astype(jnp.float32)
    angles = positions[:, None] * inv_freq[None, :]
    cosine, sine = jnp.cos(angles), jnp.sin(angles)
    return (
        jnp.concatenate([cosine, cosine], axis=-1),
        jnp.concatenate([-sine, sine], axis=-1),
    )


def shards(tokens, norm_gain, w_query, w_key, w_value, decay_rate, state_init, out_gain, w_out):
    where = lax.axis_index(SP)
    place = jnp.stack([lax.axis_index("tp_0"), lax.axis_index("tp_1"), where]).astype(jnp.int32)
    packed = jnp.concatenate([w_query, w_key, w_value, w_out.T], axis=1)
    weights = sent_to_all(packed, SP).reshape(2048, 4 * HEAD_DIM)
    normed = normalized(tokens, norm_gain)
    chunks = from_others(normed)
    cosine, sine = rotation_tables(where * (8 * BLOCK), 8 * BLOCK)
    q, local_out, sliced = local_part(place, decay_rate, chunks, weights, cosine, sine)
    out_chunks = from_others(weights[:, 3 * HEAD_DIM :])
    got = lax.all_to_all(sliced, SP, 0, 0, tiled=True)
    states = scanned(place, got, state_init.reshape(64, 2, HEAD_DIM))
    incoming = lax.all_to_all(states, SP, 0, 0, tiled=True).reshape(HEAD_DIM, HEAD_DIM)
    hidden = hidden_part(decay_rate, incoming, q, local_out, out_gain[None])
    mine = lax.all_to_all(hidden, TP, 0, 0, tiled=True)
    return out_part(place, mine, out_chunks)


def solution(mesh):
    split = Mesh(mesh.devices.reshape(8, 8, 4, 2), SP + TP)
    in_specs = (
        P(SP + TP, None),
        P(),
        P(SP, TP),
        P(SP, TP),
        P(SP, TP),
        P(SP, TP),
        P(TP, None, None),
        P(TP),
        P(TP, SP),
    )
    return jax.shard_map(
        shards, mesh=split, in_specs=in_specs, out_specs=P(SP + TP, None), check_vma=False
    )
```

```python
import jax
import jax.numpy as jnp
from jax import lax
from jax.experimental import pallas as pl
from jax.experimental.pallas import tpu as pltpu
from jax.sharding import Mesh
from jax.sharding import PartitionSpec as P


HEAD_DIM = 128
BLOCK = 128
SP = ("sp_0", "sp_1")
TP = ("tp_0", "tp_1")
ALL = SP + TP
EPS = 0.1
ROPE_BASE = 10000.0

MESSAGES = (8, HEAD_DIM + 8, HEAD_DIM)
VMEM = pl.BlockSpec(memory_space=pltpu.VMEM)
SMEM = pl.BlockSpec(memory_space=pltpu.SMEM)
ANY = pl.BlockSpec(memory_space=pl.ANY)
HBM = pl.BlockSpec(memory_space=pltpu.HBM)


def lines(first):
    groups = []
    for core in range(2):
        for fixed in range(8):
            for x in range(4):
                spots = [(fixed, m) if (core == 0) == first else (m, fixed) for m in range(8)]
                groups.append([((z * 8 + y) * 4 + x) * 2 + core for z, y in spots])
    return groups


def in_hbm(a):
    return pltpu.with_memory_space_constraint(a, pltpu.HBM)


def along(messages, first):
    return lax.all_to_all(messages, ALL, 0, 0, axis_index_groups=lines(first), tiled=True)


def shifted(own, d):
    n = lax.axis_size("tp_0")
    return lax.ppermute(own, "tp_0", [(i, (i + d) % n) for i in range(n)])


def swapped(v):
    return lax.ppermute(v, "tp_1", [(0, 1), (1, 0)])


def token_chunks(own, tables):
    same = [own] + [shifted(own, d) for d in (1, 2, 3)]
    same[2], *tables = lax.optimization_barrier((same[2], *tables))
    return same + [swapped(v) for v in same], *tables


def gather_kernel(*refs):
    chunks, out, sems = refs[:4], refs[4], refs[5]
    copies = [pltpu.make_async_copy(c, out.at[j], sems.at[j]) for j, c in enumerate(chunks)]
    for copy in copies:
        copy.start()
    for copy in copies:
        copy.wait()


def gathered(chunks):
    return pl.pallas_call(
        gather_kernel,
        out_shape=jax.ShapeDtypeStruct((4, *chunks[0].shape), chunks[0].dtype),
        in_specs=[ANY] * 4,
        out_specs=VMEM,
        scratch_shapes=[pltpu.SemaphoreType.DMA((4,))],
        compiler_params=pltpu.CompilerParams(vmem_limit_bytes=4 << 20),
        cost_estimate=pl.CostEstimate(flops=1000, bytes_accessed=4 << 20, transcendentals=0),
    )(*chunks)


def late_chunks(own):
    same = [own] + [shifted(own, d) for d in (1, 2, 3)]
    same = gathered([in_hbm(c) for c in same])
    return same, swapped(same)


def norm_kernel(x_hbm, gain_hbm, out_ref, x_ref, gain_ref, sems):
    copies = [
        pltpu.make_async_copy(x_hbm, x_ref, sems.at[0]),
        pltpu.make_async_copy(gain_hbm, gain_ref, sems.at[1]),
    ]
    for copy in copies:
        copy.start()
    for copy in copies:
        copy.wait()
    x = x_ref[...].astype(jnp.float32)
    scale = lax.rsqrt(jnp.mean(x * x, axis=-1, keepdims=True) + EPS)
    out_ref[...] = (x * scale * gain_ref[...]).astype(jnp.bfloat16)


def normalized(tokens, gain):
    return pl.pallas_call(
        norm_kernel,
        out_shape=jax.ShapeDtypeStruct(tokens.shape, jnp.bfloat16),
        in_specs=[ANY, ANY],
        out_specs=VMEM,
        scratch_shapes=[
            pltpu.VMEM(tokens.shape, tokens.dtype),
            pltpu.VMEM((1, tokens.shape[1]), gain.dtype),
            pltpu.SemaphoreType.DMA((2,)),
        ],
        compiler_params=pltpu.CompilerParams(vmem_limit_bytes=8 << 20),
        cost_estimate=pl.CostEstimate(flops=2000000, bytes_accessed=1 << 20, transcendentals=0),
    )(in_hbm(tokens), in_hbm(gain[None]))


def write_message(out, state, decay):
    row = lax.broadcasted_iota(jnp.int32, (8, HEAD_DIM), 0)
    high = decay.astype(jnp.bfloat16).astype(jnp.float32)
    rest = decay - high
    middle = rest.astype(jnp.bfloat16).astype(jnp.float32)
    addends = jnp.where(row == 0, high, jnp.where(row == 1, middle, rest - middle))
    addends = jnp.where(row < 3, addends, 0.0).astype(jnp.bfloat16)
    state = state.astype(jnp.bfloat16)
    for i in range(8):
        out[i, 0:HEAD_DIM, :] = state
        out[i, HEAD_DIM : HEAD_DIM + 8, :] = addends


def carried_on(got, here, state):
    before, shrunk = jnp.zeros_like(state), jnp.zeros((1, HEAD_DIM), jnp.float32)
    passed = jnp.ones((1, HEAD_DIM), jnp.float32)
    for j in range(8):
        mine = (here == j).astype(jnp.float32)
        decay = jnp.sum(got[j, HEAD_DIM : HEAD_DIM + 8, :].astype(jnp.float32), 0, keepdims=True)
        before = before + mine * state
        shrunk = shrunk + mine * passed
        state = decay * state + got[j, 0:HEAD_DIM, :].astype(jnp.float32)
        passed = passed * decay
    return before, shrunk, state, passed


def project_kernel(place, rates, *refs):
    xs = refs[:8]
    w_ref, cos_ref, sin_ref, q_hbm, k_hbm, v_hbm, p_hbm, o_hbm, s_out = refs[8:17]
    x_buf, q_out, k_out, v_out, p_out, sems = refs[17:]
    core = place[1]

    cut = 3 * HEAD_DIM
    copies = []
    for j in range(8):
        copies.append(pltpu.make_async_copy(xs[j], x_buf.at[pl.ds(j * BLOCK, BLOCK)], sems.at[j]))
        copies[-1].start()

    def start_row(j):
        here = lax.rem(place[0] - j % 4 + 4, 4)
        mine = core if j < 4 else 1 - core
        return pl.multiple_of((here * 2 + mine) * BLOCK, BLOCK)

    def project(block_of):
        half = 2
        for g in range(8 // half):
            for j in range(half):
                copies[g * half + j].wait()
            weights = jnp.concatenate(
                [block_of(a, b) for a in range(8) for b in range(8)], axis=0
            )
            raw = jnp.dot(
                x_buf[pl.ds(g * half * BLOCK, half * BLOCK), :],
                weights,
                preferred_element_type=jnp.float32,
            )
            for j in range(half):
                at = start_row(g * half + j)
                rows = pl.ds(at, BLOCK)
                cosine = cos_ref[rows, :]
                sine = sin_ref[rows, :]
                part = raw[j * BLOCK : (j + 1) * BLOCK, :]
                q = part[:, :HEAD_DIM]
                k = part[:, HEAD_DIM : 2 * HEAD_DIM]
                v = part[:, 2 * HEAD_DIM :]
                q = q * cosine + pltpu.roll(q, HEAD_DIM // 2, 1) * sine
                k = k * cosine + pltpu.roll(k, HEAD_DIM // 2, 1) * sine
                q_out[rows, :] = q.astype(jnp.bfloat16)
                k_out[rows, :] = k.astype(jnp.bfloat16)
                v_out[rows, :] = v.astype(jnp.bfloat16)

    @pl.when(core == 0)
    def _():
        for a in range(8):
            pltpu.make_async_copy(
                w_ref.at[a, :, :, pl.ds(cut, HEAD_DIM)], o_hbm.at[a], sems.at[9]
            ).start()
        project(lambda a, b: w_ref[a, b, :, :cut])

    @pl.when(core == 1)
    def _():
        for a in range(8):
            pltpu.make_async_copy(
                w_ref.at[:, a, :, pl.ds(cut, HEAD_DIM)], o_hbm.at[a], sems.at[9]
            ).start()
        project(lambda a, b: w_ref[b, a, :, :cut])

    leaving = [pltpu.make_async_copy(w_ref.at[:, :, :, pl.ds(cut, HEAD_DIM)], o_hbm, sems.at[9])]
    for j, (kept, out) in enumerate(((q_out, q_hbm), (k_out, k_hbm), (v_out, v_hbm))):
        leaving.append(pltpu.make_async_copy(kept, out, sems.at[j]))
        leaving[-1].start()

    row = lax.broadcasted_iota(jnp.int32, (BLOCK, BLOCK), 0).astype(jnp.float32)
    scale = HEAD_DIM**-0.5
    state = jnp.zeros((HEAD_DIM, HEAD_DIM), jnp.float32)
    total = jnp.float32(0.0)
    for b in range(8):
        rate = rates[b, 0]
        total = total + rate
        rows = pl.ds(b * BLOCK, BLOCK)
        p_out[b] = state.astype(jnp.bfloat16)
        tail = jnp.exp(-(BLOCK - 1.0 - row) * rate) * scale
        fed = (k_out[rows, :].astype(jnp.float32) * tail).astype(jnp.bfloat16)
        kv = lax.dot_general(
            fed, v_out[rows, :], (((0,), (0,)), ((), ())), preferred_element_type=jnp.float32
        )
        state = jnp.exp(jnp.full((HEAD_DIM, HEAD_DIM), -float(BLOCK), jnp.float32) * rate) * state + kv
    leaving.append(pltpu.make_async_copy(p_out, p_hbm, sems.at[3]))
    leaving[-1].start()
    write_message(s_out, state, jnp.exp(jnp.full((8, HEAD_DIM), -float(BLOCK), jnp.float32) * total))
    for copy in leaving:
        copy.wait()


def projected(place, rates, chunks, weights, cosine, sine):
    span = 8 * BLOCK
    rows = pltpu.HBM((span, HEAD_DIM), jnp.bfloat16)
    return pl.pallas_call(
        project_kernel,
        out_shape=(
            rows,
            rows,
            rows,
            pltpu.HBM((8, HEAD_DIM, HEAD_DIM), jnp.bfloat16),
            pltpu.HBM((8, 8, 32, HEAD_DIM), jnp.bfloat16),
            jax.ShapeDtypeStruct(MESSAGES, jnp.bfloat16),
        ),
        in_specs=[SMEM, SMEM] + [ANY] * 8 + [VMEM] * 3,
        out_specs=(HBM,) * 5 + (VMEM,),
        scratch_shapes=[
            pltpu.VMEM((span, 2048), jnp.bfloat16),
            pltpu.VMEM((span, HEAD_DIM), jnp.bfloat16),
            pltpu.VMEM((span, HEAD_DIM), jnp.bfloat16),
            pltpu.VMEM((span, HEAD_DIM), jnp.bfloat16),
            pltpu.VMEM((8, HEAD_DIM, HEAD_DIM), jnp.bfloat16),
            pltpu.SemaphoreType.DMA((10,)),
        ],
        compiler_params=pltpu.CompilerParams(vmem_limit_bytes=24 << 20),
        cost_estimate=pl.CostEstimate(
            flops=1700000000, bytes_accessed=7 << 20, transcendentals=1 << 18
        ),
    )(place, rates, *chunks, weights, cosine, sine)


def local_kernel(rates, q_hbm, k_hbm, v_hbm, p_hbm, l_hbm, q_ref, k_ref, v_ref, p_ref, l_out, sems):
    pairs = ((q_hbm, q_ref), (k_hbm, k_ref), (v_hbm, v_ref), (p_hbm, p_ref))
    copies = [pltpu.make_async_copy(a, b, sems.at[j]) for j, (a, b) in enumerate(pairs)]
    for copy in copies:
        copy.start()
    for copy in copies:
        copy.wait()
    row = lax.broadcasted_iota(jnp.int32, (BLOCK, BLOCK), 0).astype(jnp.float32)
    col = lax.broadcasted_iota(jnp.int32, (BLOCK, BLOCK), 1).astype(jnp.float32)
    gap = row - col
    scale = HEAD_DIM**-0.5
    for b in range(8):
        rate = rates[b, 0]
        rows = pl.ds(b * BLOCK, BLOCK)
        q, k, v = q_ref[rows, :], k_ref[rows, :], v_ref[rows, :]
        inside = jnp.where(gap >= 0.0, jnp.exp(-jnp.maximum(gap, 0.0) * rate) * scale, 0.0)
        scores = lax.dot_general(q, k, (((1,), (1,)), ((), ())), preferred_element_type=jnp.float32)
        out = jnp.dot(
            (scores * inside).astype(jnp.bfloat16), v, preferred_element_type=jnp.float32
        )
        if b > 0:
            cross = jnp.dot(q, p_ref[b], preferred_element_type=jnp.float32)
            out = out + cross * jnp.exp(-(row + 1.0) * rate)
        l_out[rows, :] = out
    leaving = pltpu.make_async_copy(l_out, l_hbm, sems.at[4])
    leaving.start()
    leaving.wait()


def local_part(rates, q, k, v, before):
    return pl.pallas_call(
        local_kernel,
        out_shape=pltpu.HBM(q.shape, jnp.float32),
        in_specs=[SMEM] + [ANY] * 4,
        out_specs=HBM,
        scratch_shapes=[
            pltpu.VMEM(q.shape, jnp.bfloat16),
            pltpu.VMEM(q.shape, jnp.bfloat16),
            pltpu.VMEM(q.shape, jnp.bfloat16),
            pltpu.VMEM(before.shape, jnp.bfloat16),
            pltpu.VMEM(q.shape, jnp.float32),
            pltpu.SemaphoreType.DMA((5,)),
        ],
        compiler_params=pltpu.CompilerParams(vmem_limit_bytes=4 << 20),
        cost_estimate=pl.CostEstimate(
            flops=1000000000, bytes_accessed=2 << 20, transcendentals=1 << 18
        ),
    )(rates, q, k, v, before)


def row_kernel(place, got, out, before_out, shrunk_out):
    zero = jnp.zeros((HEAD_DIM, HEAD_DIM), jnp.float32)
    before, shrunk, end, passed = carried_on(got, place[3], zero)
    write_message(out, end, jnp.broadcast_to(passed, (8, HEAD_DIM)))
    before_out[...] = before
    shrunk_out[...] = jnp.broadcast_to(shrunk, (8, HEAD_DIM))


def along_row(place, got):
    return pl.pallas_call(
        row_kernel,
        out_shape=(
            jax.ShapeDtypeStruct(MESSAGES, jnp.bfloat16),
            jax.ShapeDtypeStruct((HEAD_DIM, HEAD_DIM), jnp.float32),
            jax.ShapeDtypeStruct((8, HEAD_DIM), jnp.float32),
        ),
        in_specs=[SMEM, VMEM],
        out_specs=(VMEM,) * 3,
        compiler_params=pltpu.CompilerParams(vmem_limit_bytes=2 << 20),
        cost_estimate=pl.CostEstimate(flops=1000000, bytes_accessed=1 << 18, transcendentals=0),
    )(place, got)


def hidden_kernel(place, rates, got, before_ref, shrunk_ref, gain_ref, init_hbm, q_hbm, l_hbm, out_ref, *rest):
    q_ref, l_ref, init_ref, sems = rest
    pairs = ((init_hbm, init_ref), (q_hbm, q_ref), (l_hbm, l_ref))
    copies = [pltpu.make_async_copy(a, b, sems.at[j]) for j, (a, b) in enumerate(pairs)]
    for copy in copies:
        copy.start()
    copies[0].wait()
    start = carried_on(got, place[2], init_ref[...])[0]
    row = lax.broadcasted_iota(jnp.int32, (BLOCK, HEAD_DIM), 0).astype(jnp.float32)
    copies[1].wait()
    copies[2].wait()
    state = (before_ref[...] + shrunk_ref[0:1, :] * start).astype(jnp.bfloat16)
    gain = gain_ref[...]
    before = jnp.float32(0.0)
    for b in range(8):
        rate = rates[b, 0]
        rows = pl.ds(b * BLOCK, BLOCK)
        carried = jnp.dot(q_ref[rows, :], state, preferred_element_type=jnp.float32)
        mixed = l_ref[rows, :] + carried * jnp.exp(-(row + 1.0) * rate - BLOCK * before)
        norm = lax.rsqrt(jnp.mean(mixed * mixed, axis=-1, keepdims=True) + EPS)
        out_ref[b] = (mixed * norm * gain).astype(jnp.bfloat16)
        before = before + rate


def hidden_part(*args):
    return pl.pallas_call(
        hidden_kernel,
        out_shape=jax.ShapeDtypeStruct((8, BLOCK, HEAD_DIM), jnp.bfloat16),
        in_specs=[SMEM, SMEM] + [VMEM] * 4 + [ANY] * 3,
        out_specs=VMEM,
        scratch_shapes=[
            pltpu.VMEM((8 * BLOCK, HEAD_DIM), jnp.bfloat16),
            pltpu.VMEM((8 * BLOCK, HEAD_DIM), jnp.float32),
            pltpu.VMEM((HEAD_DIM, HEAD_DIM), jnp.float32),
            pltpu.SemaphoreType.DMA((3,)),
        ],
        compiler_params=pltpu.CompilerParams(vmem_limit_bytes=4 << 20),
        cost_estimate=pl.CostEstimate(
            flops=40000000, bytes_accessed=1 << 20, transcendentals=1 << 17
        ),
    )(*args)


def out_kernel(place, h_ref, same_ref, other_hbm, out_ref, other_buf, sems):
    copies = []
    for j in range(4):
        copies.append(pltpu.make_async_copy(other_hbm.at[j], other_buf.at[j], sems.at[j]))
        copies[-1].start()
    total = None
    for j in range(8):
        here = lax.rem(place[0] - j % 4 + 4, 4)
        core = place[1] if j < 4 else 1 - place[1]
        if j >= 4:
            copies[j - 4].wait()
        part = lax.dot_general(
            h_ref[here * 2 + core],
            same_ref[j] if j < 4 else other_buf[j - 4],
            (((1,), (1,)), ((), ())),
            preferred_element_type=jnp.float32,
        )
        total = part if total is None else total + part
    out_ref[...] = total.astype(jnp.bfloat16)


def out_part(place, hidden, same, other):
    return pl.pallas_call(
        out_kernel,
        out_shape=jax.ShapeDtypeStruct((BLOCK, 2048), jnp.bfloat16),
        in_specs=[SMEM, VMEM, VMEM, ANY],
        out_specs=VMEM,
        scratch_shapes=[
            pltpu.VMEM((4, 2048, HEAD_DIM), jnp.bfloat16),
            pltpu.SemaphoreType.DMA((4,)),
        ],
        compiler_params=pltpu.CompilerParams(vmem_limit_bytes=24 << 20),
        cost_estimate=pl.CostEstimate(
            flops=540000000, bytes_accessed=5 << 20, transcendentals=0
        ),
    )(place, hidden, same, other)


def rotation_tables(first, rows):
    half = HEAD_DIM // 2
    inv_freq = ROPE_BASE ** (-jnp.arange(half, dtype=jnp.float32) / half)
    positions = (first + jnp.arange(rows, dtype=jnp.int32)).astype(jnp.float32)
    angles = positions[:, None] * inv_freq[None, :]
    cosine, sine = jnp.cos(angles), jnp.sin(angles)
    return (
        jnp.concatenate([cosine, cosine], axis=-1),
        jnp.concatenate([-sine, sine], axis=-1),
    )


def shards(tokens, norm_gain, w_query, w_key, w_value, decay_rate, state_init, out_gain, w_out):
    where = lax.axis_index(SP)
    place = jnp.stack([lax.axis_index(a) for a in ("tp_0", "tp_1", "sp_0", "sp_1")]).astype(jnp.int32)
    normed = normalized(tokens, norm_gain)
    packed = jnp.concatenate([w_query, w_key, w_value, w_out.T], axis=1)[None]
    lined = along(jnp.broadcast_to(packed, (8, 32, 4 * HEAD_DIM)), True)
    tables = rotation_tables(where * (8 * BLOCK), 8 * BLOCK)
    chunks, cosine, sine = token_chunks(normed, tables)
    lined = lined.reshape(1, 256, 4 * HEAD_DIM)
    weights = along(jnp.broadcast_to(lined, (8, 256, 4 * HEAD_DIM)), False)
    weights = weights.reshape(8, 8, 32, 4 * HEAD_DIM)
    q, k, v, before, own_out, sliced = projected(place, decay_rate, chunks, weights, cosine, sine)
    out_chunks = late_chunks(own_out.reshape(2048, HEAD_DIM))
    local_out = local_part(decay_rate, in_hbm(q), in_hbm(k), in_hbm(v), in_hbm(before))
    got = lax.all_to_all(sliced, "sp_1", 0, 0, tiled=True)
    row_end, row_before, shrunk = along_row(place, got)
    got = lax.all_to_all(row_end, "sp_0", 0, 0, tiled=True)
    hidden = hidden_part(
        place,
        decay_rate,
        got,
        row_before,
        shrunk,
        out_gain[None],
        in_hbm(state_init[0]),
        in_hbm(q),
        in_hbm(local_out),
    )
    mine = lax.all_to_all(hidden, TP, 0, 0, tiled=True)
    return out_part(place, mine, *out_chunks)


def solution(mesh):
    split = Mesh(mesh.devices.reshape(8, 8, 4, 2), SP + TP)
    in_specs = (
        P(SP + TP, None),
        P(),
        P(SP, TP),
        P(SP, TP),
        P(SP, TP),
        P(SP, TP),
        P(TP, None, None),
        P(TP),
        P(TP, SP),
    )
    return jax.shard_map(
        shards, mesh=split, in_specs=in_specs, out_specs=P(SP + TP, None), check_vma=False
    )
```

```python
import jax
import jax.numpy as jnp
from jax import lax
from jax.experimental import pallas as pl
from jax.experimental.pallas import tpu as pltpu
from jax.sharding import Mesh
from jax.sharding import PartitionSpec as P


HEAD_DIM = 128
BLOCK = 128
SP = ("sp_0", "sp_1")
TP = ("tp_0", "tp_1")
ALL = SP + TP
EPS = 0.1
ROPE_BASE = 10000.0

MESSAGES = (8, HEAD_DIM + 8, HEAD_DIM)
VMEM = pl.BlockSpec(memory_space=pltpu.VMEM)
SMEM = pl.BlockSpec(memory_space=pltpu.SMEM)
ANY = pl.BlockSpec(memory_space=pl.ANY)
HBM = pl.BlockSpec(memory_space=pltpu.HBM)


def lines(first):
    groups = []
    for core in range(2):
        for fixed in range(8):
            for x in range(4):
                spots = [(fixed, m) if (core == 0) == first else (m, fixed) for m in range(8)]
                groups.append([((z * 8 + y) * 4 + x) * 2 + core for z, y in spots])
    return groups


def in_hbm(a):
    return pltpu.with_memory_space_constraint(a, pltpu.HBM)


def along(messages, first):
    return lax.all_to_all(messages, ALL, 0, 0, axis_index_groups=lines(first), tiled=True)


def shifted(own, d):
    n = lax.axis_size("tp_0")
    return lax.ppermute(own, "tp_0", [(i, (i + d) % n) for i in range(n)])


def swapped(v):
    return lax.ppermute(v, "tp_1", [(0, 1), (1, 0)])


def token_chunks(own, tables):
    same = [own] + [shifted(own, d) for d in (1, 2, 3)]
    same[2], *tables = lax.optimization_barrier((same[2], *tables))
    return same + [swapped(v) for v in same], *tables


def gather_kernel(*refs):
    chunks, out, sems = refs[:4], refs[4], refs[5]
    copies = [pltpu.make_async_copy(c, out.at[j], sems.at[j]) for j, c in enumerate(chunks)]
    for copy in copies:
        copy.start()
    for copy in copies:
        copy.wait()


def gathered(chunks):
    return pl.pallas_call(
        gather_kernel,
        out_shape=jax.ShapeDtypeStruct((4, *chunks[0].shape), chunks[0].dtype),
        in_specs=[ANY] * 4,
        out_specs=VMEM,
        scratch_shapes=[pltpu.SemaphoreType.DMA((4,))],
        compiler_params=pltpu.CompilerParams(vmem_limit_bytes=4 << 20),
        cost_estimate=pl.CostEstimate(flops=1000, bytes_accessed=4 << 20, transcendentals=0),
    )(*chunks)


def late_chunks(own):
    same = [own] + [shifted(own, d) for d in (1, 2, 3)]
    same = gathered([in_hbm(c) for c in same])
    return same, swapped(same)


def norm_kernel(x_hbm, gain_hbm, out_ref, x_ref, gain_ref, sems):
    copies = [
        pltpu.make_async_copy(x_hbm, x_ref, sems.at[0]),
        pltpu.make_async_copy(gain_hbm, gain_ref, sems.at[1]),
    ]
    for copy in copies:
        copy.start()
    for copy in copies:
        copy.wait()
    x = x_ref[...].astype(jnp.float32)
    scale = lax.rsqrt(jnp.mean(x * x, axis=-1, keepdims=True) + EPS)
    out_ref[...] = (x * scale * gain_ref[...]).astype(jnp.bfloat16)


def normalized(tokens, gain):
    return pl.pallas_call(
        norm_kernel,
        out_shape=jax.ShapeDtypeStruct(tokens.shape, jnp.bfloat16),
        in_specs=[ANY, ANY],
        out_specs=VMEM,
        scratch_shapes=[
            pltpu.VMEM(tokens.shape, tokens.dtype),
            pltpu.VMEM((1, tokens.shape[1]), gain.dtype),
            pltpu.SemaphoreType.DMA((2,)),
        ],
        compiler_params=pltpu.CompilerParams(vmem_limit_bytes=8 << 20),
        cost_estimate=pl.CostEstimate(flops=2000000, bytes_accessed=1 << 20, transcendentals=0),
    )(in_hbm(tokens), in_hbm(gain[None]))


def write_message(out, state, decay):
    row = lax.broadcasted_iota(jnp.int32, (8, HEAD_DIM), 0)
    high = decay.astype(jnp.bfloat16).astype(jnp.float32)
    rest = decay - high
    middle = rest.astype(jnp.bfloat16).astype(jnp.float32)
    addends = jnp.where(row == 0, high, jnp.where(row == 1, middle, rest - middle))
    addends = jnp.where(row < 3, addends, 0.0).astype(jnp.bfloat16)
    state = state.astype(jnp.bfloat16)
    for i in range(8):
        out[i, 0:HEAD_DIM, :] = state
        out[i, HEAD_DIM : HEAD_DIM + 8, :] = addends


def carried_on(got, here, state):
    before, shrunk = jnp.zeros_like(state), jnp.zeros((1, HEAD_DIM), jnp.float32)
    passed = jnp.ones((1, HEAD_DIM), jnp.float32)
    for j in range(8):
        mine = (here == j).astype(jnp.float32)
        decay = jnp.sum(got[j, HEAD_DIM : HEAD_DIM + 8, :].astype(jnp.float32), 0, keepdims=True)
        before = before + mine * state
        shrunk = shrunk + mine * passed
        state = decay * state + got[j, 0:HEAD_DIM, :].astype(jnp.float32)
        passed = passed * decay
    return before, shrunk, state, passed


def project_kernel(place, rates, *refs):
    xs = refs[:8]
    w_ref, cos_ref, sin_ref, q_hbm, k_hbm, v_hbm, p_hbm, o_hbm, s_hbm = refs[8:17]
    x_buf, q_out, k_out, v_out, p_out, s_out, sems = refs[17:]
    core = place[1]

    cut = 3 * HEAD_DIM
    copies = []
    for j in range(8):
        copies.append(pltpu.make_async_copy(xs[j], x_buf.at[pl.ds(j * BLOCK, BLOCK)], sems.at[j]))
        copies[-1].start()

    def start_row(j):
        here = lax.rem(place[0] - j % 4 + 4, 4)
        mine = core if j < 4 else 1 - core
        return pl.multiple_of((here * 2 + mine) * BLOCK, BLOCK)

    def project(block_of):
        half = 2
        for g in range(8 // half):
            for j in range(half):
                copies[g * half + j].wait()
            weights = jnp.concatenate(
                [block_of(a, b) for a in range(8) for b in range(8)], axis=0
            )
            raw = jnp.dot(
                x_buf[pl.ds(g * half * BLOCK, half * BLOCK), :],
                weights,
                preferred_element_type=jnp.float32,
            )
            for j in range(half):
                at = start_row(g * half + j)
                rows = pl.ds(at, BLOCK)
                cosine = cos_ref[rows, :]
                sine = sin_ref[rows, :]
                part = raw[j * BLOCK : (j + 1) * BLOCK, :]
                q = part[:, :HEAD_DIM]
                k = part[:, HEAD_DIM : 2 * HEAD_DIM]
                v = part[:, 2 * HEAD_DIM :]
                q = q * cosine + pltpu.roll(q, HEAD_DIM // 2, 1) * sine
                k = k * cosine + pltpu.roll(k, HEAD_DIM // 2, 1) * sine
                q_out[rows, :] = q.astype(jnp.bfloat16)
                k_out[rows, :] = k.astype(jnp.bfloat16)
                v_out[rows, :] = v.astype(jnp.bfloat16)

    @pl.when(core == 0)
    def _():
        for a in range(8):
            pltpu.make_async_copy(
                w_ref.at[a, :, :, pl.ds(cut, HEAD_DIM)], o_hbm.at[a], sems.at[9]
            ).start()
        project(lambda a, b: w_ref[a, b, :, :cut])

    @pl.when(core == 1)
    def _():
        for a in range(8):
            pltpu.make_async_copy(
                w_ref.at[:, a, :, pl.ds(cut, HEAD_DIM)], o_hbm.at[a], sems.at[9]
            ).start()
        project(lambda a, b: w_ref[b, a, :, :cut])

    leaving = [pltpu.make_async_copy(w_ref.at[:, :, :, pl.ds(cut, HEAD_DIM)], o_hbm, sems.at[9])]
    for j, (kept, out) in enumerate(((q_out, q_hbm), (k_out, k_hbm), (v_out, v_hbm))):
        leaving.append(pltpu.make_async_copy(kept, out, sems.at[j]))
        leaving[-1].start()

    row = lax.broadcasted_iota(jnp.int32, (BLOCK, BLOCK), 0).astype(jnp.float32)
    scale = HEAD_DIM**-0.5
    state = jnp.zeros((HEAD_DIM, HEAD_DIM), jnp.float32)
    total = jnp.float32(0.0)
    for b in range(8):
        rate = rates[b, 0]
        total = total + rate
        rows = pl.ds(b * BLOCK, BLOCK)
        p_out[b] = state.astype(jnp.bfloat16)
        tail = jnp.exp(-(BLOCK - 1.0 - row) * rate) * scale
        fed = (k_out[rows, :].astype(jnp.float32) * tail).astype(jnp.bfloat16)
        kv = lax.dot_general(
            fed, v_out[rows, :], (((0,), (0,)), ((), ())), preferred_element_type=jnp.float32
        )
        state = jnp.exp(jnp.full((HEAD_DIM, HEAD_DIM), -float(BLOCK), jnp.float32) * rate) * state + kv
    leaving.append(pltpu.make_async_copy(p_out, p_hbm, sems.at[3]))
    leaving[-1].start()
    write_message(s_out, state, jnp.exp(jnp.full((8, HEAD_DIM), -float(BLOCK), jnp.float32) * total))
    leaving.append(pltpu.make_async_copy(s_out, s_hbm, sems.at[4]))
    leaving[-1].start()
    for copy in leaving:
        copy.wait()


def projected(place, rates, chunks, weights, cosine, sine):
    span = 8 * BLOCK
    rows = pltpu.HBM((span, HEAD_DIM), jnp.bfloat16)
    return pl.pallas_call(
        project_kernel,
        out_shape=(
            rows,
            rows,
            rows,
            pltpu.HBM((8, HEAD_DIM, HEAD_DIM), jnp.bfloat16),
            pltpu.HBM((8, 8, 32, HEAD_DIM), jnp.bfloat16),
            pltpu.HBM(MESSAGES, jnp.bfloat16),
        ),
        in_specs=[SMEM, SMEM] + [ANY] * 8 + [VMEM] * 3,
        out_specs=(HBM,) * 6,
        scratch_shapes=[
            pltpu.VMEM((span, 2048), jnp.bfloat16),
            pltpu.VMEM((span, HEAD_DIM), jnp.bfloat16),
            pltpu.VMEM((span, HEAD_DIM), jnp.bfloat16),
            pltpu.VMEM((span, HEAD_DIM), jnp.bfloat16),
            pltpu.VMEM((8, HEAD_DIM, HEAD_DIM), jnp.bfloat16),
            pltpu.VMEM(MESSAGES, jnp.bfloat16),
            pltpu.SemaphoreType.DMA((10,)),
        ],
        compiler_params=pltpu.CompilerParams(vmem_limit_bytes=24 << 20),
        cost_estimate=pl.CostEstimate(
            flops=1700000000, bytes_accessed=7 << 20, transcendentals=1 << 18
        ),
    )(place, rates, *chunks, weights, cosine, sine)


def local_kernel(rates, q_hbm, k_hbm, v_hbm, p_hbm, l_hbm, q_ref, k_ref, v_ref, p_ref, l_out, sems):
    leaving = []
    pairs = ((q_hbm, q_ref), (k_hbm, k_ref), (v_hbm, v_ref), (p_hbm, p_ref))
    copies = [pltpu.make_async_copy(a, b, sems.at[j]) for j, (a, b) in enumerate(pairs)]
    for copy in copies:
        copy.start()
    for copy in copies:
        copy.wait()
    row = lax.broadcasted_iota(jnp.int32, (BLOCK, BLOCK), 0).astype(jnp.float32)
    col = lax.broadcasted_iota(jnp.int32, (BLOCK, BLOCK), 1).astype(jnp.float32)
    gap = row - col
    scale = HEAD_DIM**-0.5
    for b in range(8):
        rate = rates[b, 0]
        rows = pl.ds(b * BLOCK, BLOCK)
        q, k, v = q_ref[rows, :], k_ref[rows, :], v_ref[rows, :]
        inside = jnp.where(gap >= 0.0, jnp.exp(-jnp.maximum(gap, 0.0) * rate) * scale, 0.0)
        scores = lax.dot_general(q, k, (((1,), (1,)), ((), ())), preferred_element_type=jnp.float32)
        out = jnp.dot(
            (scores * inside).astype(jnp.bfloat16), v, preferred_element_type=jnp.float32
        )
        if b > 0:
            cross = jnp.dot(q, p_ref[b], preferred_element_type=jnp.float32)
            out = out + cross * jnp.exp(-(row + 1.0) * rate)
        l_out[rows, :] = out.astype(jnp.bfloat16)
        leaving.append(pltpu.make_async_copy(l_out.at[rows], l_hbm.at[rows], sems.at[4 + b]))
        leaving[-1].start()
    for copy in leaving:
        copy.wait()


def local_part(rates, q, k, v, before):
    return pl.pallas_call(
        local_kernel,
        out_shape=pltpu.HBM(q.shape, jnp.bfloat16),
        in_specs=[SMEM] + [ANY] * 4,
        out_specs=HBM,
        scratch_shapes=[
            pltpu.VMEM(q.shape, jnp.bfloat16),
            pltpu.VMEM(q.shape, jnp.bfloat16),
            pltpu.VMEM(q.shape, jnp.bfloat16),
            pltpu.VMEM(before.shape, jnp.bfloat16),
            pltpu.VMEM(q.shape, jnp.bfloat16),
            pltpu.SemaphoreType.DMA((12,)),
        ],
        compiler_params=pltpu.CompilerParams(vmem_limit_bytes=4 << 20),
        cost_estimate=pl.CostEstimate(
            flops=1000000000, bytes_accessed=2 << 20, transcendentals=1 << 18
        ),
    )(rates, q, k, v, before)


def row_kernel(place, got, out, before_out, shrunk_out):
    zero = jnp.zeros((HEAD_DIM, HEAD_DIM), jnp.float32)
    before, shrunk, end, passed = carried_on(got, place[3], zero)
    write_message(out, end, jnp.broadcast_to(passed, (8, HEAD_DIM)))
    before_out[...] = before
    shrunk_out[...] = jnp.broadcast_to(shrunk, (8, HEAD_DIM))


def along_row(place, got):
    return pl.pallas_call(
        row_kernel,
        out_shape=(
            jax.ShapeDtypeStruct(MESSAGES, jnp.bfloat16),
            jax.ShapeDtypeStruct((HEAD_DIM, HEAD_DIM), jnp.float32),
            jax.ShapeDtypeStruct((8, HEAD_DIM), jnp.float32),
        ),
        in_specs=[SMEM, VMEM],
        out_specs=(VMEM,) * 3,
        compiler_params=pltpu.CompilerParams(vmem_limit_bytes=2 << 20),
        cost_estimate=pl.CostEstimate(flops=1000000, bytes_accessed=1 << 18, transcendentals=0),
    )(place, got)


def hidden_kernel(place, rates, got, before_ref, shrunk_ref, gain_ref, init_hbm, q_hbm, l_hbm, out_ref, *rest):
    q_ref, l_ref, init_ref, sems = rest
    pairs = ((init_hbm, init_ref), (q_hbm, q_ref), (l_hbm, l_ref))
    copies = [pltpu.make_async_copy(a, b, sems.at[j]) for j, (a, b) in enumerate(pairs)]
    for copy in copies:
        copy.start()
    copies[0].wait()
    start = carried_on(got, place[2], init_ref[...])[0]
    row = lax.broadcasted_iota(jnp.int32, (BLOCK, HEAD_DIM), 0).astype(jnp.float32)
    copies[1].wait()
    copies[2].wait()
    state = (before_ref[...] + shrunk_ref[0:1, :] * start).astype(jnp.bfloat16)
    gain = gain_ref[...]
    before = jnp.float32(0.0)
    for b in range(8):
        rate = rates[b, 0]
        rows = pl.ds(b * BLOCK, BLOCK)
        carried = jnp.dot(q_ref[rows, :], state, preferred_element_type=jnp.float32)
        mixed = l_ref[rows, :].astype(jnp.float32) + carried * jnp.exp(-(row + 1.0) * rate - BLOCK * before)
        norm = lax.rsqrt(jnp.mean(mixed * mixed, axis=-1, keepdims=True) + EPS)
        out_ref[b] = (mixed * norm * gain).astype(jnp.bfloat16)
        before = before + rate


def hidden_part(*args):
    return pl.pallas_call(
        hidden_kernel,
        out_shape=jax.ShapeDtypeStruct((8, BLOCK, HEAD_DIM), jnp.bfloat16),
        in_specs=[SMEM, SMEM] + [VMEM] * 4 + [ANY] * 3,
        out_specs=VMEM,
        scratch_shapes=[
            pltpu.VMEM((8 * BLOCK, HEAD_DIM), jnp.bfloat16),
            pltpu.VMEM((8 * BLOCK, HEAD_DIM), jnp.bfloat16),
            pltpu.VMEM((HEAD_DIM, HEAD_DIM), jnp.float32),
            pltpu.SemaphoreType.DMA((3,)),
        ],
        compiler_params=pltpu.CompilerParams(vmem_limit_bytes=4 << 20),
        cost_estimate=pl.CostEstimate(
            flops=40000000, bytes_accessed=1 << 20, transcendentals=1 << 17
        ),
    )(*args)


def head_product(h_ref, w, place, j, own):
    here = lax.rem(place[0] - j + 4, 4)
    core = place[1] if own else 1 - place[1]
    return lax.dot_general(
        h_ref[here * 2 + core], w, (((1,), (1,)), ((), ())), preferred_element_type=jnp.float32
    )


def own_kernel(place, h_ref, same_ref, out_ref):
    out_ref[...] = sum(head_product(h_ref, same_ref[j], place, j, True) for j in range(4))


def out_kernel(place, h_ref, partial_ref, other_hbm, out_ref, other_buf, sems):
    copies = []
    for j in range(4):
        copies.append(pltpu.make_async_copy(other_hbm.at[j], other_buf.at[j], sems.at[j]))
        copies[-1].start()
    total = partial_ref[...]
    for j in range(4):
        copies[j].wait()
        total = total + head_product(h_ref, other_buf[j], place, j, False)
    out_ref[...] = total.astype(jnp.bfloat16)


def out_part(place, hidden, same, other):
    partial = pl.pallas_call(
        own_kernel,
        out_shape=jax.ShapeDtypeStruct((BLOCK, 2048), jnp.float32),
        in_specs=[SMEM, VMEM, VMEM],
        out_specs=VMEM,
        compiler_params=pltpu.CompilerParams(vmem_limit_bytes=8 << 20),
        cost_estimate=pl.CostEstimate(
            flops=270000000, bytes_accessed=3 << 20, transcendentals=0
        ),
    )(place, hidden, same)
    return pl.pallas_call(
        out_kernel,
        out_shape=jax.ShapeDtypeStruct((BLOCK, 2048), jnp.bfloat16),
        in_specs=[SMEM, VMEM, VMEM, ANY],
        out_specs=VMEM,
        scratch_shapes=[
            pltpu.VMEM((4, 2048, HEAD_DIM), jnp.bfloat16),
            pltpu.SemaphoreType.DMA((4,)),
        ],
        compiler_params=pltpu.CompilerParams(vmem_limit_bytes=16 << 20),
        cost_estimate=pl.CostEstimate(
            flops=270000000, bytes_accessed=4 << 20, transcendentals=0
        ),
    )(place, hidden, partial, other)


def rotation_tables(first, rows):
    half = HEAD_DIM // 2
    inv_freq = ROPE_BASE ** (-jnp.arange(half, dtype=jnp.float32) / half)
    positions = (first + jnp.arange(rows, dtype=jnp.int32)).astype(jnp.float32)
    angles = positions[:, None] * inv_freq[None, :]
    cosine, sine = jnp.cos(angles), jnp.sin(angles)
    return (
        jnp.concatenate([cosine, cosine], axis=-1),
        jnp.concatenate([-sine, sine], axis=-1),
    )


def shards(tokens, norm_gain, w_query, w_key, w_value, decay_rate, state_init, out_gain, w_out):
    where = lax.axis_index(SP)
    place = jnp.stack([lax.axis_index(a) for a in ("tp_0", "tp_1", "sp_0", "sp_1")]).astype(jnp.int32)
    normed = normalized(tokens, norm_gain)
    packed = jnp.concatenate([w_query, w_key, w_value, w_out.T], axis=1)[None]
    lined = along(jnp.broadcast_to(packed, (8, 32, 4 * HEAD_DIM)), True)
    tables = rotation_tables(where * (8 * BLOCK), 8 * BLOCK)
    chunks, cosine, sine = token_chunks(normed, tables)
    lined = lined.reshape(1, 256, 4 * HEAD_DIM)
    weights = along(jnp.broadcast_to(lined, (8, 256, 4 * HEAD_DIM)), False)
    weights = weights.reshape(8, 8, 32, 4 * HEAD_DIM)
    q, k, v, before, own_out, sliced = projected(place, decay_rate, chunks, weights, cosine, sine)
    out_chunks = late_chunks(own_out.reshape(2048, HEAD_DIM))
    local_out = local_part(decay_rate, in_hbm(q), in_hbm(k), in_hbm(v), in_hbm(before))
    got = lax.all_to_all(sliced, "sp_1", 0, 0, tiled=True)
    row_end, row_before, shrunk = along_row(place, got)
    got = lax.all_to_all(row_end, "sp_0", 0, 0, tiled=True)
    hidden = hidden_part(
        place,
        decay_rate,
        got,
        row_before,
        shrunk,
        out_gain[None],
        in_hbm(state_init[0]),
        in_hbm(q),
        in_hbm(local_out),
    )
    mine = lax.all_to_all(hidden, TP, 0, 0, tiled=True)
    return out_part(place, mine, *out_chunks)


def solution(mesh):
    split = Mesh(mesh.devices.reshape(8, 8, 4, 2), SP + TP)
    in_specs = (
        P(SP + TP, None),
        P(),
        P(SP, TP),
        P(SP, TP),
        P(SP, TP),
        P(SP, TP),
        P(TP, None, None),
        P(TP),
        P(TP, SP),
    )
    return jax.shard_map(
        shards, mesh=split, in_specs=in_specs, out_specs=P(SP + TP, None), check_vma=False
    )
```

```python
import jax
import jax.numpy as jnp
from jax import lax
from jax.experimental import pallas as pl
from jax.experimental.pallas import tpu as pltpu
from jax.sharding import Mesh
from jax.sharding import PartitionSpec as P


HEAD_DIM = 128
BLOCK = 128
SP = ("sp_0", "sp_1")
TP = ("tp_0", "tp_1")
ALL = SP + TP
EPS = 0.1
ROPE_BASE = 10000.0

MESSAGES = (8, HEAD_DIM + 8, HEAD_DIM)
VMEM = pl.BlockSpec(memory_space=pltpu.VMEM)
SMEM = pl.BlockSpec(memory_space=pltpu.SMEM)
ANY = pl.BlockSpec(memory_space=pl.ANY)
HBM = pl.BlockSpec(memory_space=pltpu.HBM)


def lines(first):
    groups = []
    for core in range(2):
        for fixed in range(8):
            for x in range(4):
                spots = [(fixed, m) if (core == 0) == first else (m, fixed) for m in range(8)]
                groups.append([((z * 8 + y) * 4 + x) * 2 + core for z, y in spots])
    return groups


def in_hbm(a):
    return pltpu.with_memory_space_constraint(a, pltpu.HBM)


def along(messages, first):
    return lax.all_to_all(messages, ALL, 0, 0, axis_index_groups=lines(first), tiled=True)


def shifted(own, d):
    n = lax.axis_size("tp_0")
    return lax.ppermute(own, "tp_0", [(i, (i + d) % n) for i in range(n)])


def swapped(v):
    return lax.ppermute(v, "tp_1", [(0, 1), (1, 0)])


def token_chunks(own, tables):
    same = [own] + [shifted(own, d) for d in (1, 2, 3)]
    same[2], *tables = lax.optimization_barrier((same[2], *tables))
    return same + [swapped(v) for v in same], *tables


def gather_kernel(*refs):
    chunks, out, sems = refs[:4], refs[4], refs[5]
    copies = [pltpu.make_async_copy(c, out.at[j], sems.at[j]) for j, c in enumerate(chunks)]
    for copy in copies:
        copy.start()
    for copy in copies:
        copy.wait()


def gathered(chunks):
    return pl.pallas_call(
        gather_kernel,
        out_shape=jax.ShapeDtypeStruct((4, *chunks[0].shape), chunks[0].dtype),
        in_specs=[ANY] * 4,
        out_specs=VMEM,
        scratch_shapes=[pltpu.SemaphoreType.DMA((4,))],
        compiler_params=pltpu.CompilerParams(vmem_limit_bytes=4 << 20),
        cost_estimate=pl.CostEstimate(flops=1000, bytes_accessed=4 << 20, transcendentals=0),
    )(*chunks)


def late_chunks(own):
    same = [own] + [shifted(own, d) for d in (1, 2, 3)]
    same = gathered([in_hbm(c) for c in same])
    return same, swapped(same)


def norm_kernel(x_hbm, gain_hbm, out_hbm, x_ref, gain_ref, out_ref, in_sems, out_sems, gain_sem):
    pieces = [pl.ds(j * 32, 32) for j in range(4)]
    arriving = [
        pltpu.make_async_copy(x_hbm.at[p], x_ref.at[p], in_sems.at[j]) for j, p in enumerate(pieces)
    ]
    gain_copy = pltpu.make_async_copy(gain_hbm, gain_ref, gain_sem)
    gain_copy.start()
    for copy in arriving:
        copy.start()
    gain_copy.wait()
    leaving = []
    for j, p in enumerate(pieces):
        arriving[j].wait()
        x = x_ref[p, :].astype(jnp.float32)
        scale = lax.rsqrt(jnp.mean(x * x, axis=-1, keepdims=True) + EPS)
        out_ref[p, :] = (x * scale * gain_ref[...]).astype(jnp.bfloat16)
        leaving.append(pltpu.make_async_copy(out_ref.at[p], out_hbm.at[p], out_sems.at[j]))
        leaving[-1].start()
    for copy in leaving:
        copy.wait()


def normalized(tokens, gain):
    return pl.pallas_call(
        norm_kernel,
        out_shape=pltpu.HBM(tokens.shape, jnp.bfloat16),
        in_specs=[ANY, ANY],
        out_specs=HBM,
        scratch_shapes=[
            pltpu.VMEM(tokens.shape, tokens.dtype),
            pltpu.VMEM((1, tokens.shape[1]), gain.dtype),
            pltpu.VMEM(tokens.shape, jnp.bfloat16),
            pltpu.SemaphoreType.DMA((4,)),
            pltpu.SemaphoreType.DMA((4,)),
            pltpu.SemaphoreType.DMA,
        ],
        compiler_params=pltpu.CompilerParams(vmem_limit_bytes=8 << 20),
        cost_estimate=pl.CostEstimate(flops=2000000, bytes_accessed=1 << 20, transcendentals=0),
    )(in_hbm(tokens), in_hbm(gain[None]))


def write_message(message, out, sem, state, decay):
    row = lax.broadcasted_iota(jnp.int32, (8, HEAD_DIM), 0)
    high = decay.astype(jnp.bfloat16).astype(jnp.float32)
    rest = decay - high
    middle = rest.astype(jnp.bfloat16).astype(jnp.float32)
    addends = jnp.where(row == 0, high, jnp.where(row == 1, middle, rest - middle))
    message[0:HEAD_DIM, :] = state.astype(jnp.bfloat16)
    message[HEAD_DIM : HEAD_DIM + 8, :] = jnp.where(row < 3, addends, 0.0).astype(jnp.bfloat16)
    copies = [pltpu.make_async_copy(message, out.at[i], sem.at[i]) for i in range(8)]
    for copy in copies:
        copy.start()
    return copies


def carried_on(got, here, state):
    before, shrunk = jnp.zeros_like(state), jnp.zeros((1, HEAD_DIM), jnp.float32)
    passed = jnp.ones((1, HEAD_DIM), jnp.float32)
    for j in range(8):
        mine = (here == j).astype(jnp.float32)
        decay = jnp.sum(got[j, HEAD_DIM : HEAD_DIM + 8, :].astype(jnp.float32), 0, keepdims=True)
        before = before + mine * state
        shrunk = shrunk + mine * passed
        state = decay * state + got[j, 0:HEAD_DIM, :].astype(jnp.float32)
        passed = passed * decay
    return before, shrunk, state, passed


def project_kernel(place, rates, *refs):
    xs = refs[:8]
    w_ref, cos_ref, sin_ref, q_hbm, k_hbm, v_hbm, p_hbm, o_hbm, s_hbm = refs[8:17]
    x_buf, q_out, k_out, v_out, p_out, s_out, sems = refs[17:]
    core = place[1]

    cut = 3 * HEAD_DIM
    copies = []
    for j in range(8):
        copies.append(pltpu.make_async_copy(xs[j], x_buf.at[pl.ds(j * BLOCK, BLOCK)], sems.at[j]))
        copies[-1].start()

    def start_row(j):
        here = lax.rem(place[0] - j % 4 + 4, 4)
        mine = core if j < 4 else 1 - core
        return pl.multiple_of((here * 2 + mine) * BLOCK, BLOCK)

    def project(block_of):
        half = 2
        for g in range(8 // half):
            for j in range(half):
                copies[g * half + j].wait()
            weights = jnp.concatenate(
                [block_of(a, b) for a in range(8) for b in range(8)], axis=0
            )
            raw = jnp.dot(
                x_buf[pl.ds(g * half * BLOCK, half * BLOCK), :],
                weights,
                preferred_element_type=jnp.float32,
            )
            for j in range(half):
                at = start_row(g * half + j)
                rows = pl.ds(at, BLOCK)
                cosine = cos_ref[rows, :]
                sine = sin_ref[rows, :]
                part = raw[j * BLOCK : (j + 1) * BLOCK, :]
                q = part[:, :HEAD_DIM]
                k = part[:, HEAD_DIM : 2 * HEAD_DIM]
                v = part[:, 2 * HEAD_DIM :]
                q = q * cosine + pltpu.roll(q, HEAD_DIM // 2, 1) * sine
                k = k * cosine + pltpu.roll(k, HEAD_DIM // 2, 1) * sine
                q_out[rows, :] = q.astype(jnp.bfloat16)
                k_out[rows, :] = k.astype(jnp.bfloat16)
                v_out[rows, :] = v.astype(jnp.bfloat16)

    @pl.when(core == 0)
    def _():
        for a in range(8):
            pltpu.make_async_copy(
                w_ref.at[a, :, :, pl.ds(cut, HEAD_DIM)], o_hbm.at[a], sems.at[9]
            ).start()
        project(lambda a, b: w_ref[a, b, :, :cut])

    @pl.when(core == 1)
    def _():
        for a in range(8):
            pltpu.make_async_copy(
                w_ref.at[:, a, :, pl.ds(cut, HEAD_DIM)], o_hbm.at[a], sems.at[9]
            ).start()
        project(lambda a, b: w_ref[b, a, :, :cut])

    leaving = [pltpu.make_async_copy(w_ref.at[:, :, :, pl.ds(cut, HEAD_DIM)], o_hbm, sems.at[9])]
    for j, (kept, out) in enumerate(((q_out, q_hbm), (k_out, k_hbm), (v_out, v_hbm))):
        leaving.append(pltpu.make_async_copy(kept, out, sems.at[j]))
        leaving[-1].start()

    row = lax.broadcasted_iota(jnp.int32, (BLOCK, BLOCK), 0).astype(jnp.float32)
    scale = HEAD_DIM**-0.5
    state = jnp.zeros((HEAD_DIM, HEAD_DIM), jnp.float32)
    total = jnp.float32(0.0)
    for b in range(8):
        rate = rates[b, 0]
        total = total + rate
        rows = pl.ds(b * BLOCK, BLOCK)
        p_out[b] = state.astype(jnp.bfloat16)
        tail = jnp.exp(-(BLOCK - 1.0 - row) * rate) * scale
        fed = (k_out[rows, :].astype(jnp.float32) * tail).astype(jnp.bfloat16)
        kv = lax.dot_general(
            fed, v_out[rows, :], (((0,), (0,)), ((), ())), preferred_element_type=jnp.float32
        )
        state = jnp.exp(jnp.full((HEAD_DIM, HEAD_DIM), -float(BLOCK), jnp.float32) * rate) * state + kv
    leaving.append(pltpu.make_async_copy(p_out, p_hbm, sems.at[3]))
    leaving[-1].start()
    decay = jnp.exp(jnp.full((8, HEAD_DIM), -float(BLOCK), jnp.float32) * total)
    leaving += write_message(s_out, s_hbm, sems.at[pl.ds(10, 8)], state, decay)
    for copy in leaving:
        copy.wait()


def projected(place, rates, chunks, weights, cosine, sine):
    span = 8 * BLOCK
    rows = pltpu.HBM((span, HEAD_DIM), jnp.bfloat16)
    return pl.pallas_call(
        project_kernel,
        out_shape=(
            rows,
            rows,
            rows,
            pltpu.HBM((8, HEAD_DIM, HEAD_DIM), jnp.bfloat16),
            pltpu.HBM((8, 8, 32, HEAD_DIM), jnp.bfloat16),
            pltpu.HBM(MESSAGES, jnp.bfloat16),
        ),
        in_specs=[SMEM, SMEM] + [ANY] * 8 + [VMEM] * 3,
        out_specs=(HBM,) * 6,
        scratch_shapes=[
            pltpu.VMEM((span, 2048), jnp.bfloat16),
            pltpu.VMEM((span, HEAD_DIM), jnp.bfloat16),
            pltpu.VMEM((span, HEAD_DIM), jnp.bfloat16),
            pltpu.VMEM((span, HEAD_DIM), jnp.bfloat16),
            pltpu.VMEM((8, HEAD_DIM, HEAD_DIM), jnp.bfloat16),
            pltpu.VMEM(MESSAGES[1:], jnp.bfloat16),
            pltpu.SemaphoreType.DMA((18,)),
        ],
        compiler_params=pltpu.CompilerParams(vmem_limit_bytes=24 << 20),
        cost_estimate=pl.CostEstimate(
            flops=1700000000, bytes_accessed=7 << 20, transcendentals=1 << 18
        ),
    )(place, rates, *chunks, weights, cosine, sine)


def local_kernel(rates, q_hbm, k_hbm, v_hbm, p_hbm, l_hbm, q_ref, k_ref, v_ref, p_ref, l_out, sems):
    leaving = []
    pairs = ((q_hbm, q_ref), (k_hbm, k_ref), (v_hbm, v_ref), (p_hbm, p_ref))
    copies = [pltpu.make_async_copy(a, b, sems.at[j]) for j, (a, b) in enumerate(pairs)]
    for copy in copies:
        copy.start()
    for copy in copies:
        copy.wait()
    row = lax.broadcasted_iota(jnp.int32, (BLOCK, BLOCK), 0).astype(jnp.float32)
    col = lax.broadcasted_iota(jnp.int32, (BLOCK, BLOCK), 1).astype(jnp.float32)
    gap = row - col
    scale = HEAD_DIM**-0.5
    for b in range(8):
        rate = rates[b, 0]
        rows = pl.ds(b * BLOCK, BLOCK)
        q, k, v = q_ref[rows, :], k_ref[rows, :], v_ref[rows, :]
        inside = jnp.where(gap >= 0.0, jnp.exp(-jnp.maximum(gap, 0.0) * rate) * scale, 0.0)
        scores = lax.dot_general(q, k, (((1,), (1,)), ((), ())), preferred_element_type=jnp.float32)
        out = jnp.dot(
            (scores * inside).astype(jnp.bfloat16), v, preferred_element_type=jnp.float32
        )
        if b > 0:
            cross = jnp.dot(q, p_ref[b], preferred_element_type=jnp.float32)
            out = out + cross * jnp.exp(-(row + 1.0) * rate)
        l_out[rows, :] = out.astype(jnp.bfloat16)
        leaving.append(pltpu.make_async_copy(l_out.at[rows], l_hbm.at[rows], sems.at[4 + b]))
        leaving[-1].start()
    for copy in leaving:
        copy.wait()


def local_part(rates, q, k, v, before):
    return pl.pallas_call(
        local_kernel,
        out_shape=pltpu.HBM(q.shape, jnp.bfloat16),
        in_specs=[SMEM] + [ANY] * 4,
        out_specs=HBM,
        scratch_shapes=[
            pltpu.VMEM(q.shape, jnp.bfloat16),
            pltpu.VMEM(q.shape, jnp.bfloat16),
            pltpu.VMEM(q.shape, jnp.bfloat16),
            pltpu.VMEM(before.shape, jnp.bfloat16),
            pltpu.VMEM(q.shape, jnp.bfloat16),
            pltpu.SemaphoreType.DMA((12,)),
        ],
        compiler_params=pltpu.CompilerParams(vmem_limit_bytes=4 << 20),
        cost_estimate=pl.CostEstimate(
            flops=1000000000, bytes_accessed=2 << 20, transcendentals=1 << 18
        ),
    )(rates, q, k, v, before)


def row_kernel(place, got, out, before_out, shrunk_out, message, sems):
    zero = jnp.zeros((HEAD_DIM, HEAD_DIM), jnp.float32)
    before, shrunk, end, passed = carried_on(got, place[3], zero)
    copies = write_message(message, out, sems, end, jnp.broadcast_to(passed, (8, HEAD_DIM)))
    before_out[...] = before
    shrunk_out[...] = jnp.broadcast_to(shrunk, (8, HEAD_DIM))
    for copy in copies:
        copy.wait()


def along_row(place, got):
    return pl.pallas_call(
        row_kernel,
        out_shape=(
            pltpu.HBM(MESSAGES, jnp.bfloat16),
            jax.ShapeDtypeStruct((HEAD_DIM, HEAD_DIM), jnp.float32),
            jax.ShapeDtypeStruct((8, HEAD_DIM), jnp.float32),
        ),
        in_specs=[SMEM, VMEM],
        out_specs=(HBM, VMEM, VMEM),
        scratch_shapes=[
            pltpu.VMEM(MESSAGES[1:], jnp.bfloat16),
            pltpu.SemaphoreType.DMA((8,)),
        ],
        compiler_params=pltpu.CompilerParams(vmem_limit_bytes=2 << 20),
        cost_estimate=pl.CostEstimate(flops=1000000, bytes_accessed=1 << 18, transcendentals=0),
    )(place, got)


def hidden_kernel(place, rates, got, before_ref, shrunk_ref, gain_ref, init_hbm, q_hbm, l_hbm, out_ref, *rest):
    q_ref, l_ref, init_ref, sems = rest
    pairs = ((init_hbm, init_ref), (q_hbm, q_ref), (l_hbm, l_ref))
    copies = [pltpu.make_async_copy(a, b, sems.at[j]) for j, (a, b) in enumerate(pairs)]
    for copy in copies:
        copy.start()
    copies[0].wait()
    start = carried_on(got, place[2], init_ref[...])[0]
    row = lax.broadcasted_iota(jnp.int32, (BLOCK, HEAD_DIM), 0).astype(jnp.float32)
    copies[1].wait()
    copies[2].wait()
    state = (before_ref[...] + shrunk_ref[0:1, :] * start).astype(jnp.bfloat16)
    gain = gain_ref[...]
    before = jnp.float32(0.0)
    for b in range(8):
        rate = rates[b, 0]
        rows = pl.ds(b * BLOCK, BLOCK)
        carried = jnp.dot(q_ref[rows, :], state, preferred_element_type=jnp.float32)
        mixed = l_ref[rows, :].astype(jnp.float32) + carried * jnp.exp(-(row + 1.0) * rate - BLOCK * before)
        norm = lax.rsqrt(jnp.mean(mixed * mixed, axis=-1, keepdims=True) + EPS)
        out_ref[b] = (mixed * norm * gain).astype(jnp.bfloat16)
        before = before + rate


def hidden_part(*args):
    return pl.pallas_call(
        hidden_kernel,
        out_shape=jax.ShapeDtypeStruct((8, BLOCK, HEAD_DIM), jnp.bfloat16),
        in_specs=[SMEM, SMEM] + [VMEM] * 4 + [ANY] * 3,
        out_specs=VMEM,
        scratch_shapes=[
            pltpu.VMEM((8 * BLOCK, HEAD_DIM), jnp.bfloat16),
            pltpu.VMEM((8 * BLOCK, HEAD_DIM), jnp.bfloat16),
            pltpu.VMEM((HEAD_DIM, HEAD_DIM), jnp.float32),
            pltpu.SemaphoreType.DMA((3,)),
        ],
        compiler_params=pltpu.CompilerParams(vmem_limit_bytes=4 << 20),
        cost_estimate=pl.CostEstimate(
            flops=40000000, bytes_accessed=1 << 20, transcendentals=1 << 17
        ),
    )(*args)


def head_product(h_ref, w, place, j, own):
    here = lax.rem(place[0] - j + 4, 4)
    core = place[1] if own else 1 - place[1]
    return lax.dot_general(
        h_ref[here * 2 + core], w, (((1,), (1,)), ((), ())), preferred_element_type=jnp.float32
    )


def own_kernel(place, h_ref, same_ref, out_ref):
    out_ref[...] = sum(head_product(h_ref, same_ref[j], place, j, True) for j in range(4))


def out_kernel(place, h_ref, partial_ref, other_hbm, out_ref, other_buf, sems):
    copies = []
    for j in range(4):
        copies.append(pltpu.make_async_copy(other_hbm.at[j], other_buf.at[j], sems.at[j]))
        copies[-1].start()
    total = partial_ref[...]
    for j in range(4):
        copies[j].wait()
        total = total + head_product(h_ref, other_buf[j], place, j, False)
    out_ref[...] = total.astype(jnp.bfloat16)


def out_part(place, hidden, same, other):
    partial = pl.pallas_call(
        own_kernel,
        out_shape=jax.ShapeDtypeStruct((BLOCK, 2048), jnp.float32),
        in_specs=[SMEM, VMEM, VMEM],
        out_specs=VMEM,
        compiler_params=pltpu.CompilerParams(vmem_limit_bytes=8 << 20),
        cost_estimate=pl.CostEstimate(
            flops=270000000, bytes_accessed=3 << 20, transcendentals=0
        ),
    )(place, hidden, same)
    return pl.pallas_call(
        out_kernel,
        out_shape=jax.ShapeDtypeStruct((BLOCK, 2048), jnp.bfloat16),
        in_specs=[SMEM, VMEM, VMEM, ANY],
        out_specs=VMEM,
        scratch_shapes=[
            pltpu.VMEM((4, 2048, HEAD_DIM), jnp.bfloat16),
            pltpu.SemaphoreType.DMA((4,)),
        ],
        compiler_params=pltpu.CompilerParams(vmem_limit_bytes=16 << 20),
        cost_estimate=pl.CostEstimate(
            flops=270000000, bytes_accessed=4 << 20, transcendentals=0
        ),
    )(place, hidden, partial, other)


def rotation_tables(first, rows):
    half = HEAD_DIM // 2
    inv_freq = ROPE_BASE ** (-jnp.arange(half, dtype=jnp.float32) / half)
    positions = (first + jnp.arange(rows, dtype=jnp.int32)).astype(jnp.float32)
    angles = positions[:, None] * inv_freq[None, :]
    cosine, sine = jnp.cos(angles), jnp.sin(angles)
    return (
        jnp.concatenate([cosine, cosine], axis=-1),
        jnp.concatenate([-sine, sine], axis=-1),
    )


def shards(tokens, norm_gain, w_query, w_key, w_value, decay_rate, state_init, out_gain, w_out):
    where = lax.axis_index(SP)
    place = jnp.stack([lax.axis_index(a) for a in ("tp_0", "tp_1", "sp_0", "sp_1")]).astype(jnp.int32)
    normed = normalized(tokens, norm_gain)
    packed = jnp.concatenate([w_query, w_key, w_value, w_out.T], axis=1)[None]
    lined = along(jnp.broadcast_to(packed, (8, 32, 4 * HEAD_DIM)), True)
    tables = rotation_tables(where * (8 * BLOCK), 8 * BLOCK)
    chunks, cosine, sine = token_chunks(normed, tables)
    lined = lined.reshape(1, 256, 4 * HEAD_DIM)
    weights = along(jnp.broadcast_to(lined, (8, 256, 4 * HEAD_DIM)), False)
    weights = weights.reshape(8, 8, 32, 4 * HEAD_DIM)
    q, k, v, before, own_out, sliced = projected(place, decay_rate, chunks, weights, cosine, sine)
    out_chunks = late_chunks(own_out.reshape(2048, HEAD_DIM))
    local_out = local_part(decay_rate, in_hbm(q), in_hbm(k), in_hbm(v), in_hbm(before))
    got = lax.all_to_all(sliced, "sp_1", 0, 0, tiled=True)
    row_end, row_before, shrunk = along_row(place, got)
    got = lax.all_to_all(row_end, "sp_0", 0, 0, tiled=True)
    hidden = hidden_part(
        place,
        decay_rate,
        got,
        row_before,
        shrunk,
        out_gain[None],
        in_hbm(state_init[0]),
        in_hbm(q),
        in_hbm(local_out),
    )
    mine = lax.all_to_all(hidden, TP, 0, 0, tiled=True)
    return out_part(place, mine, *out_chunks)


def solution(mesh):
    split = Mesh(mesh.devices.reshape(8, 8, 4, 2), SP + TP)
    in_specs = (
        P(SP + TP, None),
        P(),
        P(SP, TP),
        P(SP, TP),
        P(SP, TP),
        P(SP, TP),
        P(TP, None, None),
        P(TP),
        P(TP, SP),
    )
    return jax.shard_map(
        shards, mesh=split, in_specs=in_specs, out_specs=P(SP + TP, None), check_vma=False
    )
```
